32 devices in a mesh: ep: 32 (over z, y, x, core).
Axes of the slice: x: 2, y: 2, z: 4, core: 2. Of those that a mesh axis runs over, the one named last changes fastest.
Arguments:
- tokens: bfloat16 [2048, 2048], P('ep'), may hold values from -6 to 6
- conv_state: bfloat16 [2048, 3, 1024], P('ep'), may hold values from -6 to 6
- recur_state: float32 [2048, 1024], P('ep'), may hold values from -6 to 6
- w_branch: bfloat16 [2048, 1024], replicated, may hold values from -0.125 to 0.125
- w_gate: bfloat16 [2048, 1024], replicated, may hold values from -0.125 to 0.125
- conv_taps: float32 [4, 1024], replicated, may hold values from -3 to 3
- rate_blocks: bfloat16 [16, 64, 64], replicated, may hold values from -0.75 to 0.75
- input_blocks: bfloat16 [16, 64, 64], replicated, may hold values from -0.75 to 0.75
- decay_param: float32 [1024], replicated, may hold values from 1.5 to 6.5
- w_mix: bfloat16 [1024, 2048], replicated, may hold values from -0.1875 to 0.1875
- gain_pre: float32 [2048], replicated, may hold values from 0.1 to 1.9
- gain_post: float32 [2048], replicated, may hold values from 0.1 to 1.9
- gain_ffn: float32 [2048], replicated, may hold values from 0.1 to 1.9
- gain_out: float32 [2048], replicated, may hold values from 0.1 to 1.9
- routes: int32 [2048, 2], P('ep'), may hold values from 0 to 31, all different within a row; in each aligned block of 64 rows (0 to 63, 64 to 127, ...) at most 12 rows name the same one
- affinity: float32 [2048, 2], P('ep'), may hold values from 0.05 to 1
- w_expert_gate: bfloat16 [32, 2048, 512], P('ep'), may hold values from -0.125 to 0.125
- w_expert_up: bfloat16 [32, 2048, 512], P('ep'), may hold values from -0.125 to 0.125
- w_expert_down: bfloat16 [32, 512, 2048], P('ep'), may hold values from -0.25 to 0.25
Outputs:
- layer_out: bfloat16 [2048, 2048], P('ep')
- conv_next: bfloat16 [2048, 3, 1024], P('ep')
- state_next: float32 [2048, 1024], P('ep')
The draws below stay inside these ranges and needn't reach their ends.
Inputs may be any that keep to these rules, and one draw needn't show every extreme that they name: `routes`: each row names 2 different experts. Among the 64 rows of one device no expert is named more than 12 times, and in every draw some device names some expert exactly 12 times.
All inputs are finite; a program needn't handle non-finite values.
Results may differ from the reference program's by a relative error of at most 0.014.
Values may be sent and summed in bfloat16 or wider, within the bound.
A program may use at most 128 MiB of HBM per device.

```python
import math
import jax
import jax.numpy as jnp
import numpy as np
from jax import lax

D = 2048
BW = 1024
NB = 16
BS = 64
TAPS = 4
FF = 512
TOP_K = 2
SEQ_DEV = 64
TOKENS = 2048
EXPERTS = 32
CAP = 12
LIMIT = 64


def block_scale(own_key, extent, cuts, least, largest):
    def one(position, parts):
        heights = jax.random.uniform(jax.random.fold_in(jax.random.fold_in(own_key, 6), position), (parts,), jnp.float32, least / len(cuts), largest / len(cuts))
        return jnp.repeat(jnp.exp(heights), extent[position] // parts).reshape((-1,) + (1,) * (len(extent) - position - 1))

    factor_of = one(*cuts[0])
    for cut in cuts[1:]:
        factor_of = factor_of * one(*cut)
    return factor_of


def deal_out(key, own, number, rows, count, top, reach, slope):
    sequence = jax.random.permutation(key, count)
    packed, common = portions_of(count, rows * top, reach, slope, True), portions_of(count, rows * top, reach, slope, False)
    places = jnp.arange(count)

    def named(lengths, offset_by):
        used = int((lengths > 0).sum())
        fixed = max(1, used // 4)
        passed = fixed + (places - fixed + offset_by * (used - fixed)) % max(1, count - fixed)
        return jnp.zeros((count,), jnp.int32).at[sequence[jnp.where(places < fixed, places, passed)]].set(jnp.asarray(lengths, jnp.int32))

    lengths = jnp.where(number % 4 == 0, named(packed, number // 4), named(common, number - number // 4 - 1))
    mixed = jax.random.permutation(jax.random.fold_in(own, 3), count)
    donor, sink = mixed[0:count // 2 * 2:2], mixed[1:count // 2 * 2:2]
    margin = jnp.minimum(lengths[donor] - 1, reach - lengths[sink]) // 2
    margin = jnp.where((donor == sequence[0]) | (sink == sequence[0]) | (lengths[sink] == 0), 0, jnp.maximum(margin, 0))
    passed = jax.random.randint(jax.random.fold_in(own, 4), (count // 2,), 0, 1 << 20) % (margin + 1)
    lengths = lengths.at[donor].add(-passed).at[sink].add(passed)
    labels = jnp.searchsorted(jnp.cumsum(lengths), jnp.arange(rows * top), side="right").astype(jnp.int32)
    listing = labels.reshape(top, rows).T
    listing = listing[jax.random.permutation(jax.random.fold_in(own, 1), rows)]
    offset_by = jax.random.randint(jax.random.fold_in(own, 2), (rows, 1), 0, top)
    return jnp.take_along_axis(listing, (jnp.arange(top)[None, :] + offset_by) % top, axis=1)


def portions_of(count, total, reach, skew, full):
    portions = [(1 << 20) // math.isqrt(standing ** skew) + 1 for standing in range(1, count + 1)]
    largest = reach if full else min(reach, max(-(-total // count), total * portions[0] // sum(portions)))
    least = 1 if total - largest >= count - 1 else 0
    given, surplus = [largest] + [least] * (count - 1), total - largest - least * (count - 1)
    while surplus > 0:
        movable = [i for i in range(1, count) if given[i] < largest] or [i for i in range(1, count) if given[i] < reach]
        whole, left = sum([portions[i] for i in movable]), surplus
        for i in movable:
            more = min(reach - given[i], max(1, left * portions[i] // whole), surplus)
            given[i] = given[i] + more
            surplus = surplus - more
    return np.array(given)


def gaussian(own_key, dims, deviation, limit, shards=(), kind=jnp.bfloat16):
    values = jax.random.normal(own_key, dims, jnp.float32) * deviation
    if len(shards) > 0:
        values = block_scale(own_key, dims, shards, -0.22, 0.18) * values
    return jnp.clip(values, min=-limit, max=limit).astype(kind)


def setup_inputs(seed: int = 0) -> dict:
    streams_of = jax.random.split(jax.random.key(seed), 20)
    tokens = gaussian(streams_of[0], (TOKENS, D), 1.0, 6.0, ((0, 32),))
    conv_state = gaussian(streams_of[1], (TOKENS, TAPS - 1, BW), 1.0, 6.0, ((0, 32),))
    recur_state = gaussian(streams_of[2], (TOKENS, BW), 1.0, 6.0, ((0, 32),), jnp.float32)
    w_branch = gaussian(streams_of[3], (D, BW), D ** -0.5, 0.125)
    w_gate = gaussian(streams_of[4], (D, BW), D ** -0.5, 0.125)
    conv_taps = gaussian(streams_of[5], (TAPS, BW), TAPS ** -0.5, 3.0, (), jnp.float32)
    rate_blocks = gaussian(streams_of[6], (NB, BS, BS), BS ** -0.5, 0.75)
    input_blocks = gaussian(streams_of[7], (NB, BS, BS), BS ** -0.5, 0.75)
    decay_param = jnp.clip(jax.random.uniform(streams_of[8], (BW,), jnp.float32, 1.5, 6.5), 1.5, 6.5)
    w_mix = gaussian(streams_of[9], (BW, D), BW ** -0.5, 0.1875)
    gain_pre = jnp.clip(1.0 + 0.18 * jax.random.normal(streams_of[10], (D,), jnp.float32), 0.1, 1.9)
    gain_post = jnp.clip(1.0 + 0.18 * jax.random.normal(streams_of[11], (D,), jnp.float32), 0.1, 1.9)
    gain_ffn = jnp.clip(1.0 + 0.18 * jax.random.normal(streams_of[12], (D,), jnp.float32), 0.1, 1.9)
    gain_out = jnp.clip(1.0 + 0.18 * jax.random.normal(streams_of[13], (D,), jnp.float32), 0.1, 1.9)
    routes_keys = jax.random.split(jax.random.fold_in(streams_of[14], 1), TOKENS // SEQ_DEV)
    routes_turns = jax.random.permutation(jax.random.fold_in(streams_of[14], 3), TOKENS // SEQ_DEV)
    routes = jax.vmap(lambda own, number: deal_out(jax.random.fold_in(streams_of[14], 2), own, number, SEQ_DEV, EXPERTS, TOP_K, CAP, 2))(routes_keys, routes_turns).reshape((TOKENS, TOP_K))
    affinity = jnp.clip(jnp.exp(math.log(1.0) - 2.9957323 * jax.random.uniform(streams_of[15], (TOKENS, TOP_K), jnp.float32) ** block_scale(streams_of[15], (TOKENS, TOP_K), ((0, 32),), -0.2, 0.2)), 0.05, 1.0)
    w_expert_gate = gaussian(streams_of[16], (EXPERTS, D, FF), D ** -0.5, 0.125, ((0, 32),))
    w_expert_up = gaussian(streams_of[17], (EXPERTS, D, FF), D ** -0.5, 0.125, ((0, 32),))
    w_expert_down = gaussian(streams_of[18], (EXPERTS, FF, D), FF ** -0.5, 0.25, ((0, 32),))
    return dict(tokens=tokens, conv_state=conv_state, recur_state=recur_state, w_branch=w_branch, w_gate=w_gate, conv_taps=conv_taps, rate_blocks=rate_blocks, input_blocks=input_blocks, decay_param=decay_param, w_mix=w_mix, gain_pre=gain_pre, gain_post=gain_post, gain_ffn=gain_ffn, gain_out=gain_out, routes=routes, affinity=affinity, w_expert_gate=w_expert_gate, w_expert_up=w_expert_up, w_expert_down=w_expert_down)


epsilon = 1e-06
gate_scale = 8.0

def norm_rows(values, gain_vec):
    floats = values.astype(jnp.float32)
    inv_scale = lax.rsqrt(lax.optimization_barrier(jnp.mean(floats * floats, axis=-1, keepdims=True)) + epsilon)
    return floats * inv_scale * gain_vec.astype(jnp.float32)

def recurrence(tokens, conv_state, recur_state, w_branch, w_gate, conv_taps, rate_blocks, input_blocks, decay_param, w_mix, gain_pre, gain_post):
    normed = norm_rows(tokens, gain_pre).astype(jnp.bfloat16)
    branch = jnp.dot(normed, w_branch, preferred_element_type=jnp.float32).astype(jnp.bfloat16)
    gate_act = jnp.dot(normed, w_gate, preferred_element_type=jnp.float32).astype(jnp.bfloat16)
    window = jnp.concatenate([conv_state, branch[:, None, :]], axis=1)
    convolved = lax.optimization_barrier(jnp.sum(window.astype(jnp.float32) * conv_taps.astype(jnp.float32)[None], axis=1))
    row_count, branch_width = convolved.shape
    blocks = rate_blocks.shape[0]
    pieces = convolved.reshape(row_count, blocks, branch_width // blocks)
    rate_gate = jax.nn.sigmoid(jnp.einsum('snc,ncd->snd', pieces, rate_blocks.astype(jnp.float32)).reshape(row_count, branch_width))
    inflow = jax.nn.sigmoid(jnp.einsum('snc,ncd->snd', pieces, input_blocks.astype(jnp.float32)).reshape(row_count, branch_width))
    log_decay = -gate_scale * rate_gate * jax.nn.softplus(-decay_param.astype(jnp.float32))
    state_next = jnp.exp(log_decay) * recur_state + jnp.sqrt(-jnp.expm1(2.0 * log_decay)) * (inflow * convolved)
    merged = (state_next * jax.nn.gelu(gate_act.astype(jnp.float32))).astype(jnp.bfloat16)
    mix_out = jnp.dot(merged, w_mix, preferred_element_type=jnp.float32).astype(jnp.bfloat16)
    residual = tokens.astype(jnp.float32) + norm_rows(mix_out, gain_post)
    return (residual, window[:, 1:, :], state_next)

def expert_rows(bundle):
    row_block, gate_w, up_w, down_w = bundle
    gate_part = jnp.dot(row_block, gate_w, preferred_element_type=jnp.float32)
    up_part = jnp.dot(row_block, up_w, preferred_element_type=jnp.float32)
    hidden = (jax.nn.silu(gate_part) * up_part).astype(jnp.bfloat16)
    return jnp.dot(hidden, down_w, preferred_element_type=jnp.float32).astype(jnp.bfloat16)

def reference(tokens, conv_state, recur_state, w_branch, w_gate, conv_taps, rate_blocks, input_blocks, decay_param, w_mix, gain_pre, gain_post, gain_ffn, gain_out, routes, affinity, w_expert_gate, w_expert_up, w_expert_down):
    residual, conv_next, state_next = recurrence(tokens, conv_state, recur_state, w_branch, w_gate, conv_taps, rate_blocks, input_blocks, decay_param, w_mix, gain_pre, gain_post)
    ffn_in = norm_rows(residual, gain_ffn).astype(jnp.bfloat16)
    flat_routes = routes.reshape(-1).astype(jnp.int32)
    onehot = (flat_routes[:, None] == jnp.arange(EXPERTS, dtype=jnp.int32)[None, :]).astype(jnp.int32)
    rank_all = lax.optimization_barrier(jnp.sum(jnp.cumsum(onehot, axis=0) * onehot, axis=1)) - 1
    kept_rows = rank_all < LIMIT
    target = jnp.where(kept_rows, flat_routes * LIMIT + rank_all, EXPERTS * LIMIT).astype(jnp.int32)
    repeated = jnp.repeat(ffn_in, TOP_K, axis=0)
    buffer = jnp.zeros((EXPERTS * LIMIT + 1, D), jnp.bfloat16).at[target].set(repeated)
    grouped = buffer[:EXPERTS * LIMIT].reshape(EXPERTS, LIMIT, D)
    outputs = lax.map(expert_rows, (grouped, w_expert_gate, w_expert_up, w_expert_down))
    out_table = jnp.concatenate([outputs.reshape(EXPERTS * LIMIT, D), jnp.zeros((1, D), jnp.bfloat16)], axis=0)
    picked = jnp.take(out_table, target, axis=0).astype(jnp.float32).reshape(TOKENS, TOP_K, D)
    weights = affinity / lax.optimization_barrier(jnp.sum(affinity, axis=1, keepdims=True))
    combined = lax.optimization_barrier(jnp.sum(weights[:, :, None] * picked, axis=1))
    layer_out = (residual + norm_rows(combined, gain_out)).astype(jnp.bfloat16)
    return (layer_out, conv_next, state_next)
```

```python
import functools

import jax
import jax.numpy as jnp
from jax import lax
from jax.experimental import pallas as pl
from jax.experimental.pallas import tpu as pltpu
from jax.sharding import PartitionSpec as P

epsilon = 1e-06
gate_scale = 8.0
planes = 4
chunks = 4


def rms(values, gain):
    return values * lax.rsqrt(jnp.mean(values * values, axis=-1, keepdims=True) + epsilon) * gain


def mixer_kernel(
    tokens, pre, tap, recur, rate_b, input_b, slope, g_pre, g_post, g_ffn, wb_hbm, wg_hbm, wm_hbm,
    ffn_out, residual_out, branch_out, state_out,
    wb, wg, wm, normed, gate_act, merged, mix, sems,
):
    rows, width = tokens.shape
    channels = pre.shape[1]
    block = rate_b.shape[1]
    loads = [
        pltpu.make_async_copy(src, dst, sems.at[k])
        for k, (src, dst) in enumerate(((wb_hbm, wb), (wg_hbm, wg), (wm_hbm, wm)))
    ]
    for load in loads:
        load.start()
    normed[...] = rms(tokens[...].astype(jnp.float32), g_pre[...]).astype(jnp.bfloat16)
    tile = 256
    loads[0].wait()

    @pl.loop(0, channels // tile)
    def _(t):
        cols = pl.ds(pl.multiple_of(t * tile, tile), tile)
        branch_out[:, cols] = jnp.dot(
            normed[...], wb[:, cols], preferred_element_type=jnp.float32
        ).astype(jnp.bfloat16)

    loads[1].wait()

    @pl.loop(0, channels // tile)
    def _(t):
        cols = pl.ds(pl.multiple_of(t * tile, tile), tile)
        gate_act[:, cols] = jnp.dot(
            normed[...], wg[:, cols], preferred_element_type=jnp.float32
        ).astype(jnp.bfloat16)

    same = lax.broadcasted_iota(jnp.int32, (tile, tile), 0) // block == (
        lax.broadcasted_iota(jnp.int32, (tile, tile), 1) // block
    )

    def spread(ref, t):
        part = ref[pl.ds(t * tile, tile), :].astype(jnp.float32)
        return jnp.where(same, jnp.concatenate([part] * (tile // block), axis=1), 0.0).astype(
            jnp.bfloat16
        )

    for t in range(channels // tile):
        cols = pl.ds(t * tile, tile)
        conv = pre[:, cols] + branch_out[:, cols].astype(jnp.float32) * tap[:, cols]
        conv16 = conv.astype(jnp.bfloat16)
        rate = jax.nn.sigmoid(
            jnp.dot(conv16, spread(rate_b, t), preferred_element_type=jnp.float32)
        )
        inflow = jax.nn.sigmoid(
            jnp.dot(conv16, spread(input_b, t), preferred_element_type=jnp.float32)
        )
        log_decay = rate * slope[:, cols]
        decay = jnp.exp(log_decay)
        rest = -jnp.tanh(log_decay) * (decay * decay + 1.0)
        state = decay * recur[:, cols] + jnp.sqrt(rest) * (inflow * conv)
        state_out[:, cols] = state
        merged[:, cols] = (state * jax.nn.gelu(gate_act[:, cols].astype(jnp.float32))).astype(
            jnp.bfloat16
        )
    loads[2].wait()

    @pl.loop(0, width // tile)
    def _(t):
        cols = pl.ds(pl.multiple_of(t * tile, tile), tile)
        mix[:, cols] = (
            jnp.dot(merged[...], wm[:, cols], preferred_element_type=jnp.float32)
            .astype(jnp.bfloat16)
            .astype(jnp.float32)
        )

    residual = tokens[...].astype(jnp.float32) + rms(mix[...], g_post[...])
    residual_out[...] = residual
    ffn = rms(residual, g_ffn[...]).astype(jnp.bfloat16)
    part = ffn_out.shape[2]
    for c in range(ffn_out.shape[0]):
        ffn_out[c] = ffn[:, c * part : (c + 1) * part]


def experts_kernel(
    n, x, residual, code_rows, code_cols, weight_cols, g_out, wg_hbm, wu_hbm, wd_hbm,
    out,
    wg, wu, wd, xall, sbuf, rbuf, obuf, cbuf, pbuf, fbuf, total,
    load_sem, zs, zr, ds_, dr, os_, orr, ps, pr,
):
    parts, rows, part = x.shape
    group = n // planes
    slab = rbuf.shape[1] // group
    me = lax.axis_index("ep")
    plane, column = me // group, lax.rem(me, group)
    loads = [
        pltpu.make_async_copy(src.at[0], dst, load_sem.at[k])
        for k, (src, dst) in enumerate(((wg_hbm, wg), (wu_hbm, wu), (wd_hbm, wd)))
    ]
    for load in loads:
        load.start()

    def along(d):
        other = lax.rem(plane + d, planes)
        return other, other * group + column

    def beside(d):
        other = lax.rem(column + d, group)
        return other, plane * group + other

    barrier = pltpu.get_barrier_semaphore()
    for d in range(1, planes):
        pl.semaphore_signal(barrier, inc=1, device_id={"ep": along(d)[1]})
    for d in range(1, group):
        pl.semaphore_signal(barrier, inc=1, device_id={"ep": beside(d)[1]})
    pl.semaphore_wait(barrier, planes + group - 2)

    def rcopy(src, dst, send, recv, device):
        return pltpu.make_async_remote_copy(
            src_ref=src, dst_ref=dst, send_sem=send, recv_sem=recv,
            device_id={"ep": device}, device_id_type=pl.DeviceIdType.MESH,
        )

    def strip(k):
        return pl.ds(pl.multiple_of(k * slab, slab), slab)

    def seqs(k):
        return pl.ds(pl.multiple_of(k * rows, rows), rows)

    def token_copy(c, d, landing):
        other, device = along(d)
        spot = other if landing else plane
        return rcopy(
            x.at[c], xall.at[c, seqs(spot)], zs.at[c, other],
            zr.at[c, spot], device,
        )

    def slab_copy(c, d, landing, src, dst, send, recv):
        other, device = beside(d)
        spot = other if landing else column
        return rcopy(
            src.at[c, strip(other)], dst.at[c, strip(spot)], send.at[c, other],
            recv.at[c, spot], device,
        )

    def back_copy(c, d, landing):
        other, device = along(d)
        spot = other if landing else plane
        return rcopy(
            pbuf.at[c, seqs(other)], fbuf.at[c, seqs(spot)], ps.at[c, other],
            pr.at[c, spot], device,
        )

    far = list(range(1, planes))
    near = list(range(1, group))
    for c in range(parts):
        for d in far:
            token_copy(c, d, False).start()
    for c in range(parts):
        xall[c, seqs(plane)] = x[c]

    slots = rbuf.shape[1]
    lots = planes * rows
    row_at = lax.broadcasted_iota(jnp.int32, (slots, lots), 0)
    pick = jnp.zeros((slots, lots), jnp.float32)
    for k in range(code_rows.shape[0]):
        pick = jnp.where(row_at == code_rows[k : k + 1, :], 1.0, pick)
    pick = pick.astype(jnp.bfloat16)

    col_at = lax.broadcasted_iota(jnp.int32, (lots, slots), 1)
    blend = jnp.zeros((lots, slots), jnp.float32)
    for k in range(code_cols.shape[1]):
        blend = jnp.where(col_at == code_cols[:, k : k + 1], weight_cols[:, k : k + 1], blend)
    high = blend.astype(jnp.bfloat16)
    low = (blend - high.astype(jnp.float32)).astype(jnp.bfloat16)

    sums = [None, None]

    def absorb(c):
        for d in near:
            slab_copy(c, d, True, sbuf, rbuf, ds_, dr).wait_recv()
        got = rbuf[c]
        for k, w in enumerate((wg, wu)):
            piece = jnp.dot(
                got, w[c * part : (c + 1) * part, :], preferred_element_type=jnp.float32
            )
            sums[k] = piece if sums[k] is None else sums[k] + piece

    for c in range(parts):
        for d in far:
            token_copy(c, d, True).wait_recv()
        sbuf[c] = jnp.dot(pick, xall[c], preferred_element_type=jnp.float32).astype(jnp.bfloat16)
        for d in near:
            slab_copy(c, d, False, sbuf, rbuf, ds_, dr).start()
        rbuf[c, strip(column)] = sbuf[c, strip(column)]
        if c == 0:
            for load in loads:
                load.wait()
        else:
            absorb(c - 1)
    absorb(parts - 1)
    hidden = (jax.nn.silu(sums[0]) * sums[1]).astype(jnp.bfloat16)

    for c in range(parts):
        obuf[c] = jnp.dot(
            hidden, wd[:, c * part : (c + 1) * part], preferred_element_type=jnp.float32
        ).astype(jnp.bfloat16)
        for d in near:
            slab_copy(c, d, False, obuf, cbuf, os_, orr).start()
        cbuf[c, strip(column)] = obuf[c, strip(column)]

    for c in range(parts):
        for d in near:
            slab_copy(c, d, True, obuf, cbuf, os_, orr).wait_recv()
        got = cbuf[c]
        pbuf[c] = (
            jnp.dot(high, got, preferred_element_type=jnp.float32)
            + jnp.dot(low, got, preferred_element_type=jnp.float32)
        ).astype(jnp.bfloat16)
        for d in far:
            back_copy(c, d, False).start()
        fbuf[c, seqs(plane)] = pbuf[c, seqs(plane)]

    squares = jnp.zeros((rows, 1), jnp.float32)
    for c in range(parts):
        for d in far:
            back_copy(c, d, True).wait_recv()
        summed = fbuf[c, 0:rows].astype(jnp.float32)
        for q in range(1, planes):
            summed = summed + fbuf[c, q * rows : (q + 1) * rows].astype(jnp.float32)
        total[c] = summed
        squares = squares + jnp.sum(summed * summed, axis=1, keepdims=True)
    scale = lax.rsqrt(squares / (parts * part) + epsilon)
    for c in range(parts):
        cols = slice(c * part, (c + 1) * part)
        out[:, cols] = (residual[:, cols] + total[c] * scale * g_out[:, cols]).astype(out.dtype)

    for c in range(parts):
        for d in far:
            token_copy(c, d, False).wait_send()
            back_copy(c, d, False).wait_send()
        for d in near:
            slab_copy(c, d, False, sbuf, rbuf, ds_, dr).wait_send()
            slab_copy(c, d, False, obuf, cbuf, os_, orr).wait_send()


def vmem(count):
    return [pl.BlockSpec(memory_space=pltpu.VMEM)] * count


def anywhere(count):
    return [pl.BlockSpec(memory_space=pl.ANY)] * count


def shards(
    tokens, conv_state, recur_state, w_branch, w_gate, conv_taps, rate_blocks, input_blocks,
    decay_param, w_mix, gain_pre, gain_post, gain_ffn, gain_out, routes, affinity,
    w_expert_gate, w_expert_up, w_expert_down,
):
    n = lax.axis_size("ep")
    me = lax.axis_index("ep")
    rows, width = tokens.shape
    channels = recur_state.shape[1]
    top = routes.shape[1]
    hidden = w_expert_gate.shape[2]
    bf16, f32 = jnp.bfloat16, jnp.float32
    group = n // planes
    capacity = max(2, 3 * rows * top // n)
    limit = rows * top // 2
    slab = -(-planes * capacity // 16) * 16
    slots, lots, part = group * slab, planes * rows, width // chunks

    share = affinity / jnp.sum(affinity, axis=1, keepdims=True)
    info = lax.all_gather(
        jnp.concatenate([routes.astype(f32), share], axis=1), "ep", axis=0, tiled=False
    )
    everyone = info[:, :, :top].astype(jnp.int32).reshape(1, n * rows * top)
    mine = lax.dynamic_index_in_dim(
        info.reshape(planes, group, rows, 2 * top), lax.rem(me, group), 1, keepdims=False
    )
    wanted = mine[:, :, :top].astype(jnp.int32).reshape(planes * rows * top, 1)
    owner = jnp.arange(planes, dtype=jnp.int32) * group + lax.rem(me, group)
    start = jnp.repeat(owner * rows * top, rows * top)[:, None]
    index = start + jnp.tile(jnp.arange(rows * top, dtype=jnp.int32), planes)[:, None]
    place = jnp.arange(n * rows * top, dtype=jnp.int32)[None, :]
    earlier = (everyone == wanted) & (place < index)
    rank = jnp.sum(earlier.astype(jnp.int32), axis=1)
    slot = jnp.sum((earlier & (place >= start)).astype(jnp.int32), axis=1)
    expert = wanted[:, 0] - (me // group) * group
    here = (expert >= 0) & (expert < group)
    source = jnp.repeat(jnp.arange(planes, dtype=jnp.int32), rows * top)
    code = jnp.where(
        here & (rank < limit), expert * slab + source * capacity + slot, -1
    ).reshape(lots, top)
    weight = mine[:, :, top:].reshape(lots, top)

    row = lambda v: v.reshape(1, -1)
    pre = jnp.sum(conv_state.astype(f32) * conv_taps[None, :-1], axis=1)
    slope = row(-gate_scale * jax.nn.softplus(-decay_param))
    block = rate_blocks.shape[1]
    ffn, residual, branch, state_next = pl.pallas_call(
        mixer_kernel,
        out_shape=(
            jax.ShapeDtypeStruct((chunks, rows, part), bf16),
            jax.ShapeDtypeStruct((rows, width), f32),
            jax.ShapeDtypeStruct((rows, channels), bf16),
            jax.ShapeDtypeStruct((rows, channels), f32),
        ),
        in_specs=vmem(10) + anywhere(3),
        out_specs=tuple(vmem(4)),
        scratch_shapes=[
            pltpu.VMEM((width, channels), bf16),
            pltpu.VMEM((width, channels), bf16),
            pltpu.VMEM((channels, width), bf16),
            pltpu.VMEM((rows, width), bf16),
            pltpu.VMEM((rows, channels), bf16),
            pltpu.VMEM((rows, channels), bf16),
            pltpu.VMEM((rows, width), f32),
            pltpu.SemaphoreType.DMA((3,)),
        ],
        compiler_params=pltpu.CompilerParams(vmem_limit_bytes=40 << 20),
    )(
        tokens, pre, conv_taps[-1:], recur_state, rate_blocks.reshape(channels, block),
        input_blocks.reshape(channels, block), slope, row(gain_pre), row(gain_post),
        row(gain_ffn), w_branch, w_gate, w_mix,
    )
    conv_next = jnp.concatenate([conv_state[:, 1:], branch[:, None, :]], axis=1)

    dma = lambda count: pltpu.SemaphoreType.DMA((chunks, count))
    layer_out = pl.pallas_call(
        functools.partial(experts_kernel, n),
        out_shape=jax.ShapeDtypeStruct((rows, width), bf16),
        in_specs=vmem(6) + anywhere(3),
        out_specs=vmem(1)[0],
        scratch_shapes=[
            pltpu.VMEM((width, hidden), bf16),
            pltpu.VMEM((width, hidden), bf16),
            pltpu.VMEM((hidden, width), bf16),
            pltpu.VMEM((chunks, lots, part), bf16),
            pltpu.VMEM((chunks, slots, part), bf16),
            pltpu.VMEM((chunks, slots, part), bf16),
            pltpu.VMEM((chunks, slots, part), bf16),
            pltpu.VMEM((chunks, slots, part), bf16),
            pltpu.VMEM((chunks, lots, part), bf16),
            pltpu.VMEM((chunks, lots, part), bf16),
            pltpu.VMEM((chunks, rows, part), f32),
            pltpu.SemaphoreType.DMA((3,)),
            dma(planes), dma(planes), dma(group), dma(group),
            dma(group), dma(group), dma(planes), dma(planes),
        ],
        compiler_params=pltpu.CompilerParams(
            collective_id=0, has_side_effects=True, vmem_limit_bytes=48 << 20
        ),
    )(
        ffn, residual, code.T, code, weight, row(gain_out),
        w_expert_gate, w_expert_up, w_expert_down,
    )
    return (layer_out, conv_next, state_next)


def solution(mesh):
    ep, copied = "ep", P()
    return jax.shard_map(
        shards,
        mesh=mesh,
        in_specs=(P(ep, None), P(ep, None, None), P(ep, None))
        + (copied,) * 11
        + (P(ep, None),) * 2
        + (P(ep, None, None),) * 3,
        out_specs=(P(ep, None), P(ep, None, None), P(ep, None)),
        check_vma=False,
    )
```

```python
import functools

import jax
import jax.numpy as jnp
from jax import lax
from jax.experimental import pallas as pl
from jax.experimental.pallas import tpu as pltpu
from jax.sharding import PartitionSpec as P

epsilon = 1e-06
gate_scale = 8.0
planes = 4
chunks = 4


def rms(values, gain):
    return values * lax.rsqrt(jnp.mean(values * values, axis=-1, keepdims=True) + epsilon) * gain


def layer_kernel(
    n, capacity, limit, top,
    tokens, pre, tap, recur, rate_b, input_b, slope, g_pre, g_post, g_ffn, g_out, message,
    wb_hbm, wg_hbm, wm_hbm, eg_hbm, eu_hbm, ed_hbm,
    out, branch_out, state_out,
    wb, wg, wm, normed, gate_act, merged, mix, residual, mall,
    eg, eu, ed, xall, sbuf, rbuf, obuf, cbuf, pbuf, fbuf, total,
    load_sem, ms, mr, zs, zr, ds_, dr, os_, orr, ps, pr,
):
    parts, lots, part = xall.shape
    group = n // planes
    slots = rbuf.shape[1]
    slab = slots // group
    me = lax.axis_index("ep")
    plane, column = me // group, lax.rem(me, group)
    rows, width = tokens.shape
    channels = pre.shape[1]
    block = rate_b.shape[1]
    loads = [
        pltpu.make_async_copy(src, dst, load_sem.at[k])
        for k, (src, dst) in enumerate(
            (
                (wb_hbm, wb), (wg_hbm, wg), (wm_hbm, wm),
                (eg_hbm.at[0], eg), (eu_hbm.at[0], eu), (ed_hbm.at[0], ed),
            )
        )
    ]
    for load in loads:
        load.start()

    barrier = pltpu.get_barrier_semaphore()

    @pl.loop(1, n)
    def _(d):
        pl.semaphore_signal(barrier, inc=1, device_id={"ep": lax.rem(me + d, n)})

    normed[...] = rms(tokens[...].astype(jnp.float32), g_pre[...]).astype(jnp.bfloat16)
    tile = 256
    loads[0].wait()

    @pl.loop(0, channels // tile)
    def _(t):
        cols = pl.ds(pl.multiple_of(t * tile, tile), tile)
        branch_out[:, cols] = jnp.dot(
            normed[...], wb[:, cols], preferred_element_type=jnp.float32
        ).astype(jnp.bfloat16)

    def lanes(k):
        return pl.ds(pl.multiple_of(k * message.shape[1], message.shape[1]), message.shape[1])

    def message_copy(d, landing):
        device = lax.rem(me + d, n)
        spot = device if landing else me
        return pltpu.make_async_remote_copy(
            src_ref=message, dst_ref=mall.at[:, lanes(spot)], send_sem=ms.at[device],
            recv_sem=mr.at[spot], device_id={"ep": device},
            device_id_type=pl.DeviceIdType.MESH,
        )

    pl.semaphore_wait(barrier, n - 1)

    @pl.loop(1, n)
    def _(d):
        message_copy(d, False).start()

    mall[:, lanes(me)] = message[...]
    loads[1].wait()

    @pl.loop(0, channels // tile)
    def _(t):
        cols = pl.ds(pl.multiple_of(t * tile, tile), tile)
        gate_act[:, cols] = jnp.dot(
            normed[...], wg[:, cols], preferred_element_type=jnp.float32
        ).astype(jnp.bfloat16)

    same = lax.broadcasted_iota(jnp.int32, (tile, tile), 0) // block == (
        lax.broadcasted_iota(jnp.int32, (tile, tile), 1) // block
    )

    def spread(ref, t):
        part = ref[pl.ds(t * tile, tile), :].astype(jnp.float32)
        return jnp.where(same, jnp.concatenate([part] * (tile // block), axis=1), 0.0).astype(
            jnp.bfloat16
        )

    for t in range(channels // tile):
        cols = pl.ds(t * tile, tile)
        conv = pre[:, cols] + branch_out[:, cols].astype(jnp.float32) * tap[:, cols]
        conv16 = conv.astype(jnp.bfloat16)
        rate = jax.nn.sigmoid(
            jnp.dot(conv16, spread(rate_b, t), preferred_element_type=jnp.float32)
        )
        inflow = jax.nn.sigmoid(
            jnp.dot(conv16, spread(input_b, t), preferred_element_type=jnp.float32)
        )
        log_decay = rate * slope[:, cols]
        decay = jnp.exp(log_decay)
        rest = -jnp.tanh(log_decay) * (decay * decay + 1.0)
        state = decay * recur[:, cols] + jnp.sqrt(rest) * (inflow * conv)
        state_out[:, cols] = state
        merged[:, cols] = (state * jax.nn.gelu(gate_act[:, cols].astype(jnp.float32))).astype(
            jnp.bfloat16
        )
    loads[2].wait()

    @pl.loop(0, width // tile)
    def _(t):
        cols = pl.ds(pl.multiple_of(t * tile, tile), tile)
        mix[:, cols] = (
            jnp.dot(merged[...], wm[:, cols], preferred_element_type=jnp.float32)
            .astype(jnp.bfloat16)
            .astype(jnp.float32)
        )

    residual[...] = tokens[...].astype(jnp.float32) + rms(mix[...], g_post[...])
    ffn = rms(residual[...], g_ffn[...]).astype(jnp.bfloat16)
    own = pl.ds(pl.multiple_of(plane * rows, rows), rows)
    for c in range(parts):
        xall[c, own] = ffn[:, c * part : (c + 1) * part]

    def along(d):
        other = lax.rem(plane + d, planes)
        return other, other * group + column

    def beside(d):
        other = lax.rem(column + d, group)
        return other, plane * group + other

    def rcopy(src, dst, send, recv, device):
        return pltpu.make_async_remote_copy(
            src_ref=src, dst_ref=dst, send_sem=send, recv_sem=recv,
            device_id={"ep": device}, device_id_type=pl.DeviceIdType.MESH,
        )

    def strip(k):
        return pl.ds(pl.multiple_of(k * slab, slab), slab)

    def seqs(k):
        return pl.ds(pl.multiple_of(k * rows, rows), rows)

    def token_copy(c, d, landing):
        other, device = along(d)
        spot = other if landing else plane
        return rcopy(
            xall.at[c, seqs(plane)], xall.at[c, seqs(spot)], zs.at[c, other],
            zr.at[c, spot], device,
        )

    def slab_copy(c, d, landing, src, dst, send, recv):
        other, device = beside(d)
        spot = other if landing else column
        return rcopy(
            src.at[c, strip(other)], dst.at[c, strip(spot)], send.at[c, other],
            recv.at[c, spot], device,
        )

    def back_copy(c, d, landing):
        other, device = along(d)
        spot = other if landing else plane
        return rcopy(
            pbuf.at[c, seqs(other)], fbuf.at[c, seqs(spot)], ps.at[c, other],
            pr.at[c, spot], device,
        )

    far = list(range(1, planes))
    near = list(range(1, group))
    for c in range(parts):
        for d in far:
            token_copy(c, d, False).start()

    @pl.loop(1, n)
    def _(d):
        message_copy(d, True).wait_recv()

    f32 = jnp.float32
    names = lax.broadcasted_iota(jnp.int32, (group, 1), 0)
    named = (names + plane * group).astype(f32)
    every = jnp.zeros((group, mall.shape[1]), f32)
    for k in range(top):
        every = every + jnp.where(mall[k : k + 1, :] == named, 1.0, 0.0)
    device_at = lax.broadcasted_iota(jnp.int32, every.shape, 1) // message.shape[1]
    lot_at = lax.broadcasted_iota(jnp.int32, (1, lots), 1)
    base = jnp.zeros((group, lots), f32)
    current = []
    for q in range(planes):
        device = q * group + column
        before = jnp.sum(jnp.where(device_at < device, every, 0.0), axis=1, keepdims=True)
        base = jnp.where(lot_at // rows == q, before, base)
        current.append(mall[:, lanes(device)][:, :rows])
    current = jnp.concatenate(current, axis=1)
    one = [jnp.where(current[k : k + 1, :] == named, 1.0, 0.0) for k in range(top)]
    left = lax.broadcasted_iota(jnp.int32, (lots, lots), 0)
    right = lax.broadcasted_iota(jnp.int32, (lots, lots), 1)
    upper = jnp.where((left // rows == right // rows) & (left < right), 1.0, 0.0)
    slot = jnp.dot(
        sum(one).astype(jnp.bfloat16), upper.astype(jnp.bfloat16), preferred_element_type=f32
    )
    spot_of = jnp.where(
        base + slot < limit,
        (names * slab + (lot_at // rows) * capacity + 1).astype(f32) + slot,
        0.0,
    )
    codes = [jnp.sum(one[k] * spot_of, axis=0, keepdims=True) - 1.0 for k in range(top)]
    raw = [current[top + k : top + k + 1, :] for k in range(top)]
    shares = [r / sum(raw) for r in raw]
    spare = [jnp.zeros((1, lots), f32)] * (-2 * top % 8)
    turned = jnp.transpose(jnp.concatenate(codes + shares + spare, axis=0))

    row_at = lax.broadcasted_iota(jnp.int32, (slots, lots), 0).astype(f32)
    pick = jnp.zeros((slots, lots), f32)
    for k in range(top):
        pick = jnp.where(row_at == codes[k], 1.0, pick)
    pick = pick.astype(jnp.bfloat16)
    col_at = lax.broadcasted_iota(jnp.int32, (lots, slots), 1).astype(f32)
    blend = jnp.zeros((lots, slots), f32)
    for k in range(top):
        blend = jnp.where(
            col_at == turned[:, k : k + 1], turned[:, top + k : top + k + 1], blend
        )
    high = blend.astype(jnp.bfloat16)
    low = (blend - high.astype(f32)).astype(jnp.bfloat16)

    sums = [None, None]

    def absorb(c):
        for d in near:
            slab_copy(c, d, True, sbuf, rbuf, ds_, dr).wait_recv()
        got = rbuf[c]
        for k, w in enumerate((eg, eu)):
            piece = jnp.dot(
                got, w[c * part : (c + 1) * part, :], preferred_element_type=jnp.float32
            )
            sums[k] = piece if sums[k] is None else sums[k] + piece

    for c in range(parts):
        for d in far:
            token_copy(c, d, True).wait_recv()
        sbuf[c] = jnp.dot(pick, xall[c], preferred_element_type=jnp.float32).astype(jnp.bfloat16)
        for d in near:
            slab_copy(c, d, False, sbuf, rbuf, ds_, dr).start()
        rbuf[c, strip(column)] = sbuf[c, strip(column)]
        if c == 0:
            for load in loads[3:]:
                load.wait()
        else:
            absorb(c - 1)
    absorb(parts - 1)
    hidden = (jax.nn.silu(sums[0]) * sums[1]).astype(jnp.bfloat16)

    for c in range(parts):
        obuf[c] = jnp.dot(
            hidden, ed[:, c * part : (c + 1) * part], preferred_element_type=jnp.float32
        ).astype(jnp.bfloat16)
        for d in near:
            slab_copy(c, d, False, obuf, cbuf, os_, orr).start()
        cbuf[c, strip(column)] = obuf[c, strip(column)]

    for c in range(parts):
        for d in near:
            slab_copy(c, d, True, obuf, cbuf, os_, orr).wait_recv()
        got = cbuf[c]
        pbuf[c] = (
            jnp.dot(high, got, preferred_element_type=jnp.float32)
            + jnp.dot(low, got, preferred_element_type=jnp.float32)
        ).astype(jnp.bfloat16)
        for d in far:
            back_copy(c, d, False).start()
        fbuf[c, seqs(plane)] = pbuf[c, seqs(plane)]

    squares = jnp.zeros((rows, 1), jnp.float32)
    for c in range(parts):
        for d in far:
            back_copy(c, d, True).wait_recv()
        summed = fbuf[c, 0:rows].astype(jnp.float32)
        for q in range(1, planes):
            summed = summed + fbuf[c, q * rows : (q + 1) * rows].astype(jnp.float32)
        total[c] = summed
        squares = squares + jnp.sum(summed * summed, axis=1, keepdims=True)
    scale = lax.rsqrt(squares / (parts * part) + epsilon)
    for c in range(parts):
        cols = slice(c * part, (c + 1) * part)
        out[:, cols] = (residual[:, cols] + total[c] * scale * g_out[:, cols]).astype(out.dtype)

    @pl.loop(1, n)
    def _(d):
        message_copy(d, False).wait_send()

    for c in range(parts):
        for d in far:
            token_copy(c, d, False).wait_send()
            back_copy(c, d, False).wait_send()
        for d in near:
            slab_copy(c, d, False, sbuf, rbuf, ds_, dr).wait_send()
            slab_copy(c, d, False, obuf, cbuf, os_, orr).wait_send()


def vmem(count):
    return [pl.BlockSpec(memory_space=pltpu.VMEM)] * count


def anywhere(count):
    return [pl.BlockSpec(memory_space=pl.ANY)] * count


def shards(
    tokens, conv_state, recur_state, w_branch, w_gate, conv_taps, rate_blocks, input_blocks,
    decay_param, w_mix, gain_pre, gain_post, gain_ffn, gain_out, routes, affinity,
    w_expert_gate, w_expert_up, w_expert_down,
):
    n = lax.axis_size("ep")
    rows, width = tokens.shape
    channels = recur_state.shape[1]
    top = routes.shape[1]
    hidden = w_expert_gate.shape[2]
    bf16, f32 = jnp.bfloat16, jnp.float32
    group = n // planes
    capacity = max(2, 3 * rows * top // n)
    limit = rows * top // 2
    slab = -(-planes * capacity // 16) * 16
    slots, lots, part = group * slab, planes * rows, width // chunks

    message = jnp.concatenate([routes.T.astype(f32), affinity.T], axis=0)
    message = jnp.pad(
        message, ((0, -2 * top % 8), (0, -rows % 128)), constant_values=-1.0
    )

    row = lambda v: v.reshape(1, -1)
    pre = jnp.sum(conv_state.astype(f32) * conv_taps[None, :-1], axis=1)
    slope = row(-gate_scale * jax.nn.softplus(-decay_param))
    block = rate_blocks.shape[1]
    dma = lambda *count: pltpu.SemaphoreType.DMA(count)
    layer_out, branch, state_next = pl.pallas_call(
        functools.partial(layer_kernel, n, capacity, limit, top),
        out_shape=(
            jax.ShapeDtypeStruct((rows, width), bf16),
            jax.ShapeDtypeStruct((rows, channels), bf16),
            jax.ShapeDtypeStruct((rows, channels), f32),
        ),
        in_specs=vmem(12) + anywhere(6),
        out_specs=tuple(vmem(3)),
        scratch_shapes=[
            pltpu.VMEM((width, channels), bf16),
            pltpu.VMEM((width, channels), bf16),
            pltpu.VMEM((channels, width), bf16),
            pltpu.VMEM((rows, width), bf16),
            pltpu.VMEM((rows, channels), bf16),
            pltpu.VMEM((rows, channels), bf16),
            pltpu.VMEM((rows, width), f32),
            pltpu.VMEM((rows, width), f32),
            pltpu.VMEM((message.shape[0], n * message.shape[1]), f32),
            pltpu.VMEM((width, hidden), bf16),
            pltpu.VMEM((width, hidden), bf16),
            pltpu.VMEM((hidden, width), bf16),
            pltpu.VMEM((chunks, lots, part), bf16),
            pltpu.VMEM((chunks, slots, part), bf16),
            pltpu.VMEM((chunks, slots, part), bf16),
            pltpu.VMEM((chunks, slots, part), bf16),
            pltpu.VMEM((chunks, slots, part), bf16),
            pltpu.VMEM((chunks, lots, part), bf16),
            pltpu.VMEM((chunks, lots, part), bf16),
            pltpu.VMEM((chunks, rows, part), f32),
            dma(6), dma(n), dma(n),
            dma(chunks, planes), dma(chunks, planes), dma(chunks, group), dma(chunks, group),
            dma(chunks, group), dma(chunks, group), dma(chunks, planes), dma(chunks, planes),
        ],
        compiler_params=pltpu.CompilerParams(
            collective_id=0, has_side_effects=True, vmem_limit_bytes=60 << 20
        ),
    )(
        tokens, pre, conv_taps[-1:], recur_state, rate_blocks.reshape(channels, block),
        input_blocks.reshape(channels, block), slope, row(gain_pre), row(gain_post),
        row(gain_ffn), row(gain_out), message,
        w_branch, w_gate, w_mix, w_expert_gate, w_expert_up, w_expert_down,
    )
    conv_next = jnp.concatenate([conv_state[:, 1:], branch[:, None, :]], axis=1)
    return (layer_out, conv_next, state_next)


def solution(mesh):
    ep, copied = "ep", P()
    return jax.shard_map(
        shards,
        mesh=mesh,
        in_specs=(P(ep, None), P(ep, None, None), P(ep, None))
        + (copied,) * 11
        + (P(ep, None),) * 2
        + (P(ep, None, None),) * 3,
        out_specs=(P(ep, None), P(ep, None, None), P(ep, None)),
        check_vma=False,
    )
```

```python
import functools

import jax
import jax.numpy as jnp
from jax import lax
from jax.experimental import pallas as pl
from jax.experimental.pallas import tpu as pltpu
from jax.sharding import PartitionSpec as P

epsilon = 1e-06
gate_scale = 8.0
planes = 4
chunks = 4


def rms(values, gain):
    return values * lax.rsqrt(jnp.mean(values * values, axis=-1, keepdims=True) + epsilon) * gain


def layer_kernel(
    n, capacity, limit, top,
    tokens, pre, taps, recur, rate_b, input_b, decay_p, g_pre, g_post, g_ffn, g_out, routes, affinity,
    wb_hbm, wg_hbm, wm_hbm, eg_hbm, eu_hbm, ed_hbm,
    out, branch_out, state_out,
    wb, wg, wm, normed, gate_act, merged, mix, residual, message, mall,
    eg, eu, ed, xall, sbuf, rbuf, obuf, cbuf, pbuf, fbuf, total,
    load_sem, ms, mr, zs, zr, ds_, dr, os_, orr, ps, pr,
):
    parts, lots, part = xall.shape
    group = n // planes
    slots = rbuf.shape[1]
    slab = slots // group
    me = lax.axis_index("ep")
    plane, column = me // group, lax.rem(me, group)
    rows, width = tokens.shape
    channels = pre.shape[1]
    block = rate_b.shape[1]
    loads = [
        pltpu.make_async_copy(src, dst, load_sem.at[k])
        for k, (src, dst) in enumerate(
            (
                (wb_hbm, wb), (wg_hbm, wg), (wm_hbm, wm),
                (eg_hbm.at[0], eg), (eu_hbm.at[0], eu), (ed_hbm.at[0], ed),
            )
        )
    ]
    for load in loads:
        load.start()

    barrier = pltpu.get_barrier_semaphore()

    @pl.loop(1, n)
    def _(d):
        pl.semaphore_signal(barrier, inc=1, device_id={"ep": lax.rem(me + d, n)})

    normed[...] = rms(tokens[...].astype(jnp.float32), g_pre[...]).astype(jnp.bfloat16)
    tile = 256
    loads[0].wait()

    @pl.loop(0, channels // tile)
    def _(t):
        cols = pl.ds(pl.multiple_of(t * tile, tile), tile)
        branch_out[:, cols] = jnp.dot(
            normed[...], wb[:, cols], preferred_element_type=jnp.float32
        ).astype(jnp.bfloat16)

    def lanes(k):
        return pl.ds(pl.multiple_of(k * message.shape[1], message.shape[1]), message.shape[1])

    def message_copy(d, landing):
        device = lax.rem(me + d, n)
        spot = device if landing else me
        return pltpu.make_async_remote_copy(
            src_ref=message, dst_ref=mall.at[:, lanes(spot)], send_sem=ms.at[device],
            recv_sem=mr.at[spot], device_id={"ep": device},
            device_id_type=pl.DeviceIdType.MESH,
        )

    spots = lax.broadcasted_iota(jnp.int32, (rows, message.shape[1]), 1)
    wide = jnp.full((rows, message.shape[1]), -1.0, jnp.float32)
    for k in range(top):
        wide = jnp.where(spots == k, routes[:, k : k + 1].astype(jnp.float32), wide)
        wide = jnp.where(spots == top + k, affinity[:, k : k + 1], wide)
    message[...] = jnp.full(message.shape, -1.0, jnp.float32)
    message[:, :rows] = jnp.transpose(wide)[: message.shape[0]]
    pl.semaphore_wait(barrier, n - 1)

    @pl.loop(1, n)
    def _(d):
        message_copy(d, False).start()

    mall[:, lanes(me)] = message[...]
    loads[1].wait()

    @pl.loop(0, channels // tile)
    def _(t):
        cols = pl.ds(pl.multiple_of(t * tile, tile), tile)
        gate_act[:, cols] = jnp.dot(
            normed[...], wg[:, cols], preferred_element_type=jnp.float32
        ).astype(jnp.bfloat16)

    same = lax.broadcasted_iota(jnp.int32, (tile, tile), 0) // block == (
        lax.broadcasted_iota(jnp.int32, (tile, tile), 1) // block
    )

    def spread(ref, t):
        part = ref[pl.ds(t * tile, tile), :].astype(jnp.float32)
        return jnp.where(same, jnp.concatenate([part] * (tile // block), axis=1), 0.0).astype(
            jnp.bfloat16
        )

    for t in range(channels // tile):
        cols = pl.ds(t * tile, tile)
        conv = pre[:, cols] + branch_out[:, cols].astype(jnp.float32) * taps[taps.shape[0] - 1 :, cols]
        conv16 = conv.astype(jnp.bfloat16)
        rate = jax.nn.sigmoid(
            jnp.dot(conv16, spread(rate_b, t), preferred_element_type=jnp.float32)
        )
        inflow = jax.nn.sigmoid(
            jnp.dot(conv16, spread(input_b, t), preferred_element_type=jnp.float32)
        )
        log_decay = rate * (-gate_scale * jax.nn.softplus(-decay_p[:, cols]))
        decay = jnp.exp(log_decay)
        rest = -jnp.tanh(log_decay) * (decay * decay + 1.0)
        state = decay * recur[:, cols] + jnp.sqrt(rest) * (inflow * conv)
        state_out[:, cols] = state
        merged[:, cols] = (state * jax.nn.gelu(gate_act[:, cols].astype(jnp.float32))).astype(
            jnp.bfloat16
        )
    loads[2].wait()

    @pl.loop(0, width // tile)
    def _(t):
        cols = pl.ds(pl.multiple_of(t * tile, tile), tile)
        mix[:, cols] = (
            jnp.dot(merged[...], wm[:, cols], preferred_element_type=jnp.float32)
            .astype(jnp.bfloat16)
            .astype(jnp.float32)
        )

    residual[...] = tokens[...].astype(jnp.float32) + rms(mix[...], g_post[...])
    ffn = rms(residual[...], g_ffn[...]).astype(jnp.bfloat16)
    own = pl.ds(pl.multiple_of(plane * rows, rows), rows)
    for c in range(parts):
        xall[c, own] = ffn[:, c * part : (c + 1) * part]

    def along(d):
        other = lax.rem(plane + d, planes)
        return other, other * group + column

    def beside(d):
        other = lax.rem(column + d, group)
        return other, plane * group + other

    def rcopy(src, dst, send, recv, device):
        return pltpu.make_async_remote_copy(
            src_ref=src, dst_ref=dst, send_sem=send, recv_sem=recv,
            device_id={"ep": device}, device_id_type=pl.DeviceIdType.MESH,
        )

    def strip(k):
        return pl.ds(pl.multiple_of(k * slab, slab), slab)

    def seqs(k):
        return pl.ds(pl.multiple_of(k * rows, rows), rows)

    def token_hop(c, origin, up):
        return rcopy(
            xall.at[c, seqs(origin)], xall.at[c, seqs(origin)],
            zs.at[c, origin + (planes if up else 0)], zr.at[c, origin],
            lax.rem(me + (group if up else n - group), n),
        )

    def each_hop(c, step):
        for up in (True, False):
            open_end = plane + 1 < planes if up else plane > 0
            for h in range(planes):
                origin = plane - h if up else plane + h
                held = origin >= 0 if up else origin < planes

                @pl.when(open_end & held)
                def _():
                    step(token_hop(c, origin, up))

    def own_hops(c):
        for up in (True, False):

            @pl.when(plane + 1 < planes if up else plane > 0)
            def _():
                token_hop(c, plane, up).start()

    def pass_on(c):
        for h in range(1, planes):
            for up in (True, False):
                origin = plane - h if up else plane + h

                @pl.when(origin >= 0 if up else origin < planes)
                def _():
                    token_hop(c, origin, up).wait_recv()

                    @pl.when(plane + 1 < planes if up else plane > 0)
                    def _():
                        token_hop(c, origin, up).start()

    def slab_copy(c, d, landing, src, dst, send, recv):
        other, device = beside(d)
        spot = other if landing else column
        return rcopy(
            src.at[c, strip(other)], dst.at[c, strip(spot)], send.at[c, other],
            recv.at[c, spot], device,
        )

    def back_copy(c, d, landing):
        other, device = along(d)
        spot = other if landing else plane
        return rcopy(
            pbuf.at[c, seqs(other)], fbuf.at[c, seqs(spot)], ps.at[c, other],
            pr.at[c, spot], device,
        )

    far = list(range(1, planes))
    near = list(range(1, group))
    ahead = 2
    for c in range(min(ahead, parts)):
        own_hops(c)

    @pl.loop(1, n)
    def _(d):
        message_copy(d, True).wait_recv()

    f32 = jnp.float32
    names = lax.broadcasted_iota(jnp.int32, (group, 1), 0)
    named = (names + plane * group).astype(f32)
    every = jnp.zeros((group, mall.shape[1]), f32)
    for k in range(top):
        every = every + jnp.where(mall[k : k + 1, :] == named, 1.0, 0.0)
    device_at = lax.broadcasted_iota(jnp.int32, every.shape, 1) // message.shape[1]
    lot_at = lax.broadcasted_iota(jnp.int32, (1, lots), 1)
    base = jnp.zeros((group, lots), f32)
    current = []
    for q in range(planes):
        device = q * group + column
        before = jnp.sum(jnp.where(device_at < device, every, 0.0), axis=1, keepdims=True)
        base = jnp.where(lot_at // rows == q, before, base)
        current.append(mall[:, lanes(device)][:, :rows])
    current = jnp.concatenate(current, axis=1)
    one = [jnp.where(current[k : k + 1, :] == named, 1.0, 0.0) for k in range(top)]
    left = lax.broadcasted_iota(jnp.int32, (lots, lots), 0)
    right = lax.broadcasted_iota(jnp.int32, (lots, lots), 1)
    upper = jnp.where((left // rows == right // rows) & (left < right), 1.0, 0.0)
    slot = jnp.dot(
        sum(one).astype(jnp.bfloat16), upper.astype(jnp.bfloat16), preferred_element_type=f32
    )
    spot_of = jnp.where(
        base + slot < limit,
        (names * slab + (lot_at // rows) * capacity + 1).astype(f32) + slot,
        0.0,
    )
    codes = [jnp.sum(one[k] * spot_of, axis=0, keepdims=True) - 1.0 for k in range(top)]
    raw = [current[top + k : top + k + 1, :] for k in range(top)]
    shares = [r / sum(raw) for r in raw]
    spare = [jnp.zeros((1, lots), f32)] * (-2 * top % 8)
    turned = jnp.transpose(jnp.concatenate(codes + shares + spare, axis=0))

    row_at = lax.broadcasted_iota(jnp.int32, (slots, lots), 0).astype(f32)
    pick = jnp.zeros((slots, lots), f32)
    for k in range(top):
        pick = jnp.where(row_at == codes[k], 1.0, pick)
    pick = pick.astype(jnp.bfloat16)
    col_at = lax.broadcasted_iota(jnp.int32, (lots, slots), 1).astype(f32)
    blend = jnp.zeros((lots, slots), f32)
    for k in range(top):
        blend = jnp.where(
            col_at == turned[:, k : k + 1], turned[:, top + k : top + k + 1], blend
        )
    high = blend.astype(jnp.bfloat16)
    low = (blend - high.astype(f32)).astype(jnp.bfloat16)

    sums = [None, None]

    def absorb(c):
        for d in near:
            slab_copy(c, d, True, sbuf, rbuf, ds_, dr).wait_recv()
        got = rbuf[c]
        for k, w in enumerate((eg, eu)):
            piece = jnp.dot(
                got, w[c * part : (c + 1) * part, :], preferred_element_type=jnp.float32
            )
            sums[k] = piece if sums[k] is None else sums[k] + piece

    for c in range(parts):
        pass_on(c)
        if c + ahead < parts:
            own_hops(c + ahead)
        sbuf[c] = jnp.dot(pick, xall[c], preferred_element_type=jnp.float32).astype(jnp.bfloat16)
        for d in near:
            slab_copy(c, d, False, sbuf, rbuf, ds_, dr).start()
        rbuf[c, strip(column)] = sbuf[c, strip(column)]
        if c == 0:
            for load in loads[3:]:
                load.wait()
        else:
            absorb(c - 1)
    absorb(parts - 1)
    hidden = (jax.nn.silu(sums[0]) * sums[1]).astype(jnp.bfloat16)

    for c in range(parts):
        obuf[c] = jnp.dot(
            hidden, ed[:, c * part : (c + 1) * part], preferred_element_type=jnp.float32
        ).astype(jnp.bfloat16)
        for d in near:
            slab_copy(c, d, False, obuf, cbuf, os_, orr).start()
        cbuf[c, strip(column)] = obuf[c, strip(column)]

    for c in range(parts):
        for d in near:
            slab_copy(c, d, True, obuf, cbuf, os_, orr).wait_recv()
        got = cbuf[c]
        pbuf[c] = (
            jnp.dot(high, got, preferred_element_type=jnp.float32)
            + jnp.dot(low, got, preferred_element_type=jnp.float32)
        ).astype(jnp.bfloat16)
        for d in far:
            back_copy(c, d, False).start()
        fbuf[c, seqs(plane)] = pbuf[c, seqs(plane)]

    squares = jnp.zeros((rows, 1), jnp.float32)
    for c in range(parts):
        for d in far:
            back_copy(c, d, True).wait_recv()
        summed = fbuf[c, 0:rows].astype(jnp.float32)
        for q in range(1, planes):
            summed = summed + fbuf[c, q * rows : (q + 1) * rows].astype(jnp.float32)
        total[c] = summed
        squares = squares + jnp.sum(summed * summed, axis=1, keepdims=True)
    scale = lax.rsqrt(squares / (parts * part) + epsilon)
    for c in range(parts):
        cols = slice(c * part, (c + 1) * part)
        out[:, cols] = (residual[:, cols] + total[c] * scale * g_out[:, cols]).astype(out.dtype)

    @pl.loop(1, n)
    def _(d):
        message_copy(d, False).wait_send()

    for c in range(parts):
        each_hop(c, lambda hop: hop.wait_send())
        for d in far:
            back_copy(c, d, False).wait_send()
        for d in near:
            slab_copy(c, d, False, sbuf, rbuf, ds_, dr).wait_send()
            slab_copy(c, d, False, obuf, cbuf, os_, orr).wait_send()


def vmem(count):
    return [pl.BlockSpec(memory_space=pltpu.VMEM)] * count


def anywhere(count):
    return [pl.BlockSpec(memory_space=pl.ANY)] * count


def shards(
    tokens, conv_state, recur_state, w_branch, w_gate, conv_taps, rate_blocks, input_blocks,
    decay_param, w_mix, gain_pre, gain_post, gain_ffn, gain_out, routes, affinity,
    w_expert_gate, w_expert_up, w_expert_down,
):
    n = lax.axis_size("ep")
    rows, width = tokens.shape
    channels = recur_state.shape[1]
    top = routes.shape[1]
    hidden = w_expert_gate.shape[2]
    bf16, f32 = jnp.bfloat16, jnp.float32
    group = n // planes
    capacity = max(2, 3 * rows * top // n)
    limit = rows * top // 2
    slab = -(-planes * capacity // 16) * 16
    slots, lots, part = group * slab, planes * rows, width // chunks

    row = lambda v: v.reshape(1, -1)
    pre = jnp.sum(conv_state.astype(f32) * conv_taps[None, :-1], axis=1)
    letter = (-(-2 * top // 8) * 8, -(-rows // 128) * 128)
    block = rate_blocks.shape[1]
    dma = lambda *count: pltpu.SemaphoreType.DMA(count)
    layer_out, branch, state_next = pl.pallas_call(
        functools.partial(layer_kernel, n, capacity, limit, top),
        out_shape=(
            jax.ShapeDtypeStruct((rows, width), bf16),
            jax.ShapeDtypeStruct((rows, channels), bf16),
            jax.ShapeDtypeStruct((rows, channels), f32),
        ),
        in_specs=vmem(13) + anywhere(6),
        out_specs=tuple(vmem(3)),
        scratch_shapes=[
            pltpu.VMEM((width, channels), bf16),
            pltpu.VMEM((width, channels), bf16),
            pltpu.VMEM((channels, width), bf16),
            pltpu.VMEM((rows, width), bf16),
            pltpu.VMEM((rows, channels), bf16),
            pltpu.VMEM((rows, channels), bf16),
            pltpu.VMEM((rows, width), f32),
            pltpu.VMEM((rows, width), f32),
            pltpu.VMEM(letter, f32),
            pltpu.VMEM((letter[0], n * letter[1]), f32),
            pltpu.VMEM((width, hidden), bf16),
            pltpu.VMEM((width, hidden), bf16),
            pltpu.VMEM((hidden, width), bf16),
            pltpu.VMEM((chunks, lots, part), bf16),
            pltpu.VMEM((chunks, slots, part), bf16),
            pltpu.VMEM((chunks, slots, part), bf16),
            pltpu.VMEM((chunks, slots, part), bf16),
            pltpu.VMEM((chunks, slots, part), bf16),
            pltpu.VMEM((chunks, lots, part), bf16),
            pltpu.VMEM((chunks, lots, part), bf16),
            pltpu.VMEM((chunks, rows, part), f32),
            dma(6), dma(n), dma(n),
            dma(chunks, 2 * planes), dma(chunks, planes), dma(chunks, group), dma(chunks, group),
            dma(chunks, group), dma(chunks, group), dma(chunks, planes), dma(chunks, planes),
        ],
        compiler_params=pltpu.CompilerParams(
            collective_id=0, has_side_effects=True, vmem_limit_bytes=60 << 20
        ),
    )(
        tokens, pre, conv_taps, recur_state, rate_blocks.reshape(channels, block),
        input_blocks.reshape(channels, block), row(decay_param), row(gain_pre), row(gain_post),
        row(gain_ffn), row(gain_out), routes, affinity,
        w_branch, w_gate, w_mix, w_expert_gate, w_expert_up, w_expert_down,
    )
    conv_next = jnp.concatenate([conv_state[:, 1:], branch[:, None, :]], axis=1)
    return (layer_out, conv_next, state_next)


def solution(mesh):
    ep, copied = "ep", P()
    return jax.shard_map(
        shards,
        mesh=mesh,
        in_specs=(P(ep, None), P(ep, None, None), P(ep, None))
        + (copied,) * 11
        + (P(ep, None),) * 2
        + (P(ep, None, None),) * 3,
        out_specs=(P(ep, None), P(ep, None, None), P(ep, None)),
        check_vma=False,
    )
```
